32 devices in a mesh: ep: 8 (over z, core), tp: 4 (over y, x).
Axes of the slice: x: 2, y: 2, z: 4, core: 2. Of those that a mesh axis runs over, the one named last changes fastest.
Arguments:
- tokens: bfloat16 [1024, 2048], P('ep', 'tp')
- norm_gain: float32 [2048], P('tp'), may hold values from 0.1 to 1.9
- routing: int32 [1024, 2], P('ep'), may hold values from 0 to 3, all different within a row; in each aligned block of 128 rows (0 to 127, 128 to 255, ...) at most 80 rows name the same one
- route_weight: float32 [1024, 2], P('ep'), may hold values from 0.1 to 1
- gate_weight: bfloat16 [8, 2048, 3584], P('ep', None, 'tp'), may hold values from -0.125 to 0.125
- up_weight: bfloat16 [8, 2048, 3584], P('ep', None, 'tp'), may hold values from -0.125 to 0.125
- down_weight: bfloat16 [8, 3584, 2048], P('ep', None, 'tp')
- final_gain: float32 [2048], P('tp'), may hold values from 0.1 to 1.9
Outputs:
- mixed: bfloat16 [1024, 2048], P('ep', 'tp')
The draws below stay inside these ranges and needn't reach their ends.
Inputs may be any that keep to these rules, and one draw needn't show every extreme that they name: `routing`: each row names 2 different experts. Among the 128 rows of one device along ep (aligned blocks), no expert is named more than 80 times, a bound that some blocks reach.
All inputs are finite; a program needn't handle non-finite values.
Results may differ from the reference program's by a relative error of at most 0.0077.
Values may be sent and summed in bfloat16 or wider, within the bound.
A program may use at most 64 MiB of HBM per device.

```python
import math
import jax
import jax.numpy as jnp
import numpy as np
from jax import lax

D = 2048
FF = 7168
TOPK = 2
TOK_DEV = 128
EXPERTS = 4
CAP = 80
TOKENS = 1024
N_EP = 8


def draw_tokens(key, part):
    column = jnp.arange(D, dtype=jnp.float32) / D
    values = jax.random.normal(key, (TOKENS, D), jnp.float32) * 10.0 ** (0.8 * column)
    return values.astype(jnp.bfloat16)


def draw_down_weight(key, part):
    column = jnp.arange(D, dtype=jnp.float32) / D
    scale = (FF // 2) ** (-0.5) * 10.0 ** (0.8 * column)
    values = jax.random.normal(key, (2 * EXPERTS, FF // 2, D), jnp.float32)
    return (values * scale).astype(jnp.bfloat16)


def block_scale(rng, dims, cuts, low, high):
    level, own = 1.0, jax.random.fold_in(rng, 6)
    for position, shards_of in cuts:
        steps = jnp.exp(jax.random.uniform(jax.random.fold_in(own, position), (shards_of,), jnp.float32, low / len(cuts), high / len(cuts)))
        level = level * jnp.repeat(steps, dims[position] // shards_of).reshape([-1 if axis == position else 1 for axis in range(len(dims))])
    return level


def shared_out(own_key, own, number, rows, count, top, most, lean):
    order = jax.random.permutation(own_key, count)
    crowded, usual = portions_of(count, rows * top, most, lean, True), portions_of(count, rows * top, most, lean, False)
    places = jnp.arange(count)

    def named(sizes, rotation):
        used = int((sizes > 0).sum())
        fixed = max(1, used // 4)
        passed = fixed + (places - fixed + rotation * (used - fixed)) % max(1, count - fixed)
        return jnp.zeros((count,), jnp.int32).at[order[jnp.where(places < fixed, places, passed)]].set(jnp.asarray(sizes, jnp.int32))

    sizes = jnp.where(number % 4 == 0, named(crowded, number // 4), named(usual, number - number // 4 - 1))
    mixed = jax.random.permutation(jax.random.fold_in(own, 3), count)
    source_of, receiver = mixed[0:count // 2 * 2:2], mixed[1:count // 2 * 2:2]
    room = jnp.minimum(sizes[source_of] - 1, most - sizes[receiver]) // 2
    room = jnp.where((source_of == order[0]) | (receiver == order[0]) | (sizes[receiver] == 0), 0, jnp.maximum(room, 0))
    passed = jax.random.randint(jax.random.fold_in(own, 4), (count // 2,), 0, 1 << 20) % (room + 1)
    sizes = sizes.at[source_of].add(-passed).at[receiver].add(passed)
    members = jnp.searchsorted(jnp.cumsum(sizes), jnp.arange(rows * top), side="right").astype(jnp.int32)
    grid = members.reshape(top, rows).T
    grid = grid[jax.random.permutation(jax.random.fold_in(own, 1), rows)]
    rotation = jax.random.randint(jax.random.fold_in(own, 2), (rows, 1), 0, top)
    return jnp.take_along_axis(grid, (jnp.arange(top)[None, :] + rotation) % top, axis=1)


def portions_of(amount, total, limit, lean, full):
    portions = [(1 << 20) // math.isqrt(standing ** lean) + 1 for standing in range(1, amount + 1)]
    largest = limit if full else min(limit, max(-(-total // amount), total * portions[0] // sum(portions)))
    least = 1 if total - largest >= amount - 1 else 0
    given, surplus = [largest] + [least] * (amount - 1), total - largest - least * (amount - 1)
    while surplus > 0:
        movable = [i for i in range(1, amount) if given[i] < largest] or [i for i in range(1, amount) if given[i] < limit]
        pool, budget = sum([portions[i] for i in movable]), surplus
        for i in movable:
            extra = min(limit - given[i], max(1, budget * portions[i] // pool), surplus)
            given[i] = given[i] + extra
            surplus = surplus - extra
    return np.array(given)


def scatter_about(key, extent, deviation, most, shards=(), held_as=jnp.bfloat16):
    array = jax.random.normal(key, extent, jnp.float32) * deviation
    if len(shards) > 0:
        array = block_scale(key, extent, shards, -0.22, 0.18) * array
    return jnp.clip(array, min=-most, max=most).astype(held_as)


def setup_inputs(seed: int = 0) -> dict:
    seeds = jax.random.split(jax.random.key(seed), 9)
    tokens = draw_tokens(jax.random.fold_in(seeds[8], 71), 0)
    norm_gain = jnp.clip(1.0 + 0.18 * jax.random.normal(seeds[1], (D,), jnp.float32), 0.1, 1.9)
    routing_keys = jax.random.split(jax.random.fold_in(seeds[2], 1), TOKENS // TOK_DEV)
    routing_turns = jax.random.permutation(jax.random.fold_in(seeds[2], 3), TOKENS // TOK_DEV)
    routing = jax.vmap(lambda own, number: shared_out(jax.random.fold_in(seeds[2], 2), own, number, TOK_DEV, EXPERTS, TOPK, CAP, 2))(routing_keys, routing_turns).reshape((TOKENS, TOPK))
    route_weight = jnp.clip(0.1 + 0.9 * jax.random.uniform(seeds[3], (TOKENS, TOPK), jnp.float32) ** block_scale(seeds[3], (TOKENS, TOPK), ((0, 8),), -0.2, 0.2), 0.1, 1.0)
    gate_weight = scatter_about(seeds[4], (2 * EXPERTS, D, FF // 2), D ** -0.5, 0.125, ((0, 8), (2, 4)))
    up_weight = scatter_about(seeds[5], (2 * EXPERTS, D, FF // 2), D ** -0.5, 0.125, ((0, 8), (2, 4)))
    down_weight = draw_down_weight(jax.random.fold_in(seeds[8], 71), 0)
    final_gain = jnp.clip(1.0 + 0.18 * jax.random.normal(seeds[7], (D,), jnp.float32), 0.1, 1.9)
    return dict(tokens=tokens, norm_gain=norm_gain, routing=routing, route_weight=route_weight, gate_weight=gate_weight, up_weight=up_weight, down_weight=down_weight, final_gain=final_gain)


EPS = 1e-05

def rms_scale(values, gain):
    return values * lax.rsqrt(lax.optimization_barrier(jnp.mean(values * values, axis=-1, keepdims=True)) + EPS) * gain

def slot_numbers(expert_ids):
    onehot = (expert_ids[..., None] == jnp.arange(EXPERTS, dtype=jnp.int32)).astype(jnp.int32)
    before = jnp.cumsum(onehot, axis=1) - onehot
    return lax.optimization_barrier(jnp.sum(before * onehot, axis=2)).astype(jnp.int32)

def reference(tokens, norm_gain, routing, route_weight, gate_weight, up_weight, down_weight, final_gain):
    normed = rms_scale(tokens.astype(jnp.float32), norm_gain).astype(jnp.bfloat16)
    copies = TOK_DEV * TOPK
    expert_ids = routing.reshape(N_EP, copies).astype(jnp.int32)
    slot_index = slot_numbers(expert_ids)
    source_index = jnp.broadcast_to(jnp.arange(N_EP, dtype=jnp.int32)[:, None], (N_EP, copies))
    token_index = jnp.broadcast_to((jnp.arange(copies, dtype=jnp.int32) // TOPK)[None, :], (N_EP, copies))
    source_rows = normed.reshape(N_EP, TOK_DEV, D)[source_index, token_index]

    def one_expert(expert):
        target = jnp.where(expert_ids == expert, slot_index, CAP)
        buffer = jnp.zeros((N_EP, CAP, D), jnp.bfloat16).at[source_index, target].set(source_rows, mode='drop')
        buffer = buffer.reshape(N_EP * CAP, D)
        results = []
        for half_index in range(2):
            row = 2 * expert + half_index
            gate_half = lax.dynamic_index_in_dim(gate_weight, row, 0, keepdims=False)
            up_half = lax.dynamic_index_in_dim(up_weight, row, 0, keepdims=False)
            down_half = lax.dynamic_index_in_dim(down_weight, row, 0, keepdims=False)
            gate = jnp.dot(buffer, gate_half, preferred_element_type=jnp.float32)
            upper = jnp.dot(buffer, up_half, preferred_element_type=jnp.float32)
            hidden = (jax.nn.silu(gate) * upper).astype(jnp.bfloat16)
            results.append(jnp.dot(hidden, down_half, preferred_element_type=jnp.float32).astype(jnp.bfloat16))
        return jnp.stack(results)
    results = lax.map(one_expert, jnp.arange(EXPERTS, dtype=jnp.int32))
    results = results.reshape(EXPERTS, 2, N_EP, CAP, D)
    picked = results[expert_ids, :, source_index, slot_index]
    paired = (picked[:, :, 0].astype(jnp.float32) + picked[:, :, 1].astype(jnp.float32)).astype(jnp.bfloat16)
    paired = lax.optimization_barrier(paired)
    summed = paired.astype(jnp.float32)
    weights = route_weight.reshape(N_EP, copies).astype(jnp.float32)
    mixed_sum = lax.optimization_barrier(jnp.sum((summed * weights[..., None]).reshape(N_EP, TOK_DEV, TOPK, D), axis=2))
    mixed_sum = mixed_sum.reshape(TOKENS, D)
    return rms_scale(mixed_sum, final_gain).astype(jnp.bfloat16)
```

```python
import functools

import jax
import jax.numpy as jnp
from jax import lax
from jax.experimental import pallas as pl
from jax.experimental.pallas import tpu as pltpu
from jax.sharding import PartitionSpec as P

TOPK = 2
EPS = 1e-05
MESH = pl.DeviceIdType.MESH
F32, BF16 = jnp.float32, jnp.bfloat16


def flipped(index, mask):
    out, bit = index, 1
    while bit <= mask:
        if mask & bit:
            out = out + bit - 2 * bit * ((index // bit) % 2)
        bit *= 2
    return out


def dot(a, b):
    return jnp.dot(a, b, preferred_element_type=F32)


def kernel(
    n, planes, groups,
    tokens, gain, routing, routing_t, route_weight, gate_hbm, up_hbm, down_hbm, final_gain,
    out,
    wg, wu, wd, gains, picked, x, xn, hid, half_own, half_send, half_recv, pair, comb, sq_out, sq_in,
    w_sem, gain_s, gain_r, disp_s, disp_r, x_s, x_r, d2d_s, d2d_r, h_s, h_r, po_s, po_r, c_s, c_r,
    sq_s, sq_r,
):
    ep, t = lax.axis_index("ep"), lax.axis_index("tp")
    z, core = ep // 2, ep % 2
    partner = (ep + 1 - 2 * core, t)
    cap, width = picked.shape[1], picked.shape[2]
    per = planes // groups
    rows = per * cap
    inner = hid.shape[-1]
    tok_rows = tokens.shape[0]
    depth = n * width
    bits = [1 << b for b in range(n.bit_length() - 1)]
    tp_peer = [(ep, flipped(t, j)) for j in range(n)]
    tp_index = [flipped(t, j) for j in range(n)]
    expert = [flipped(z, k) for k in range(planes)]
    plane_peer = [(2 * expert[k] + core, t) for k in range(planes)]

    loads = [
        pltpu.make_async_copy(src.at[0], dst, w_sem.at[i])
        for i, (src, dst) in enumerate(((gate_hbm, wg), (up_hbm, wu), (down_hbm, wd)))
    ]
    for load in loads:
        load.start()

    barrier = pltpu.get_barrier_semaphore()
    peers = tp_peer[1:] + plane_peer[1:] + [partner]
    for peer in peers:
        pl.semaphore_signal(barrier, inc=1, device_id=peer, device_id_type=MESH)

    token_row = lax.broadcasted_iota(jnp.int32, (tok_rows, tok_rows), 0)
    token_col = lax.broadcasted_iota(jnp.int32, (tok_rows, tok_rows), 1)
    r_t0, r_t1 = routing_t[0:1, :], routing_t[1:2, :]
    wide = -(-planes // 16) * 16
    sub = lax.broadcasted_iota(jnp.int32, (wide, tok_rows), 0)
    member_t = jnp.zeros((wide, tok_rows), F32)
    for k in range(planes):
        named = ((r_t0 == expert[k]) | (r_t1 == expert[k])).astype(F32)
        member_t = jnp.where(sub == k, named, member_t)
    earlier = (token_row < token_col).astype(F32).astype(BF16)
    slot_t = dot(member_t.astype(BF16), earlier)
    slot_t = jnp.where(member_t > 0, slot_t, -1.0)
    slot_sub = lax.broadcasted_iota(jnp.int32, (cap, tok_rows), 0).astype(F32)

    def pick(k):
        chosen = (slot_sub == slot_t[k : k + 1, :]).astype(F32).astype(BF16)
        return dot(chosen, tokens[...]).astype(BF16)

    sent = []

    def remote(src, dst, s, r, peer):
        return pltpu.make_async_remote_copy(
            src_ref=src, dst_ref=dst, send_sem=s, recv_sem=r, device_id=peer, device_id_type=MESH
        )

    def start(copy):
        copy.start()
        sent.append(copy)
        return copy

    for k in range(1, planes):
        picked[k] = pick(k)
    x[0, 0, 0, 0] = pick(0)

    pl.semaphore_wait(barrier, len(peers))

    disp = [
        None if k == 0 else remote(
            picked.at[k], x.at[k // per, 0, 0, k % per], disp_s.at[k], disp_r.at[k], plane_peer[k]
        )
        for k in range(planes)
    ]
    for k in range(1, planes):
        start(disp[k])

    def tree(at, send_sem, recv_sem, order):
        copies, need = {}, {0: []}
        have = [0]
        for position, bit in enumerate(order):
            for j in list(have):
                into = j ^ bit
                copies[into] = remote(at(j), at(into), send_sem(into), recv_sem(into), tp_peer[bit])
                need[j].append(into)
                need[into] = []
                have.append(into)
        return copies, need, have[1:]

    def ascending(g):
        return bits if g % 2 == 0 else bits[::-1]

    trees = [
        tree(
            lambda j, g=g: x.at[g, j, 0], lambda j, g=g: x_s.at[g, j],
            lambda j, g=g: x_r.at[g, j], ascending(g),
        )
        for g in range(groups)
    ]
    across = [
        [remote(x.at[g, j, 0], x.at[g, j, 1], d2d_s.at[g, j], d2d_r.at[g, j], partner) for j in range(n)]
        for g in range(groups)
    ]
    hidden_trees = [
        [
            tree(
                lambda j, g=g, side=side: hid.at[g, j, side],
                lambda j, g=g, side=side: h_s.at[g, side, j],
                lambda j, g=g, side=side: h_r.at[g, side, j], ascending(side),
            )
            for side in range(2)
        ]
        for g in range(groups)
    ]

    def gather_start(g):
        for k in range(max(1, g * per), (g + 1) * per):
            disp[k].wait_recv()
        copies, need, _ = trees[g]
        for into in need[0]:
            start(copies[into])
        start(across[g][0])

    def gather_relay(g):
        copies, need, arrivals = trees[g]
        for j in arrivals:
            if need[j]:
                copies[j].wait_recv()
                for into in need[j]:
                    start(copies[into])
                start(across[g][j])

    def gather_end(g):
        copies, need, arrivals = trees[g]
        for j in arrivals:
            if not need[j]:
                copies[j].wait_recv()
                start(across[g][j])
        for j in range(n):
            across[g][j].wait_recv()

    def upward(g):
        parts = [x[g, j].reshape(2 * rows, width).astype(F32) for j in range(n)]
        square = sum(jnp.sum(p * p, axis=1, keepdims=True) for p in parts)
        scale = lax.rsqrt(square / depth + EPS)
        for j in range(n):
            columns = pl.ds(pl.multiple_of(tp_index[j] * width, width), width)
            xn[:, columns] = (parts[j] * scale * gains[j]).astype(BF16)
        for first in range(0, inner, 256):
            last = min(first + 256, inner)
            left = dot(xn[...], wg[:, first:last])
            right = dot(xn[...], wu[:, first:last])
            value = (jax.nn.silu(left) * right).astype(BF16)
            hid[g, 0, :, :, first:last] = value.reshape(2, rows, last - first)
        for step in range(len(bits)):
            for side in range(2):
                copies, need, _ = hidden_trees[g][side]
                start(copies[need[0][step]])

    def hidden_relay(g):
        for side in range(2):
            copies, need, arrivals = hidden_trees[g][side]
            for j in arrivals:
                if need[j]:
                    copies[j].wait_recv()
                    for into in need[j]:
                        start(copies[into])

    halves = [
        remote(half_send.at[g], half_recv.at[g], po_s.at[g], po_r.at[g], partner) for g in range(groups)
    ]

    def downward(g):
        for side in range(2):
            copies, need, arrivals = hidden_trees[g][side]
            for j in arrivals:
                if not need[j]:
                    copies[j].wait_recv()
        total = None
        for j in range(n):
            part = wd[pl.ds(pl.multiple_of(tp_index[j] * inner, inner), inner), :]
            term = dot(hid[g, j].reshape(2 * rows, inner), part)
            total = term if total is None else total + term
        half_own[g] = total[:rows].astype(BF16)
        half_send[g] = total[rows:].astype(BF16)
        start(halves[g])

    back = [
        None if k == 0 else remote(
            pair.at[k // per, k % per], comb.at[k], c_s.at[k], c_r.at[k], plane_peer[k]
        )
        for k in range(planes)
    ]

    def combine(g):
        halves[g].wait_recv()
        both = (half_own[g].astype(F32) + half_recv[g].astype(F32)).astype(BF16)
        pair[g] = both.reshape(per, cap, width)
        for k in range(g * per, (g + 1) * per):
            if k == 0:
                comb[0] = both[:cap]
            else:
                start(back[k])

    gather_start(0)
    gain_copies = [
        remote(gain, gains.at[j], gain_s.at[j], gain_r.at[j], tp_peer[j]) for j in range(1, n)
    ]
    for copy in gain_copies:
        start(copy)
    gains[0] = gain[...]
    if groups > 1:
        gather_start(1)
    gather_relay(0)
    for copy in gain_copies:
        copy.wait_recv()
    loads[0].wait()
    loads[1].wait()
    for g in range(groups):
        gather_end(g)
        upward(g)
        if g == 0:
            for later in range(2, groups):
                gather_start(later)
            loads[2].wait()
        if g + 1 < groups:
            gather_relay(g + 1)
        if g >= 1:
            hidden_relay(g - 1)
        if g >= 2:
            downward(g - 2)
        if g >= 3:
            combine(g - 3)
    hidden_relay(groups - 1)
    for g in range(max(0, groups - 2), groups):
        downward(g)
        if g >= 1:
            combine(g - 1)

    lane = lax.broadcasted_iota(jnp.int32, (tok_rows, 128), 1)
    r_0, r_1 = routing[:, 0:1], routing[:, 1:2]
    member = jnp.zeros((tok_rows, 128), F32)
    for k in range(planes):
        named = ((r_0 == expert[k]) | (r_1 == expert[k])).astype(F32)
        member = jnp.where(lane == k, named, member)
    before = (token_col < token_row).astype(F32).astype(BF16)
    slot = dot(before, member.astype(BF16))
    slot_lane = lax.broadcasted_iota(jnp.int32, (tok_rows, cap), 1).astype(F32)
    w_0, w_1 = route_weight[:, 0:1], route_weight[:, 1:2]

    def share(k):
        weight = jnp.where(r_0 == expert[k], w_0, jnp.where(r_1 == expert[k], w_1, 0.0))
        table = jnp.where(slot_lane == slot[:, k : k + 1], weight, 0.0)
        high = table.astype(BF16)
        rest = table - high.astype(F32)
        middle = rest.astype(BF16)
        low = (rest - middle.astype(F32)).astype(BF16)
        block = comb[k]
        return dot(high, block) + (dot(middle, block) + dot(low, block))

    combine(groups - 1)
    mixed = share(0)
    for k in range(1, planes):
        back[k].wait_recv()
        mixed = mixed + share(k)

    square = jnp.sum(mixed * mixed, axis=1, keepdims=True)
    sq_out[...] = jnp.transpose(jnp.broadcast_to(square, (tok_rows, 128)))[0:8, :]
    sums = [remote(sq_out, sq_in.at[j], sq_s.at[j], sq_r.at[j], tp_peer[j]) for j in range(1, n)]
    for copy in sums:
        start(copy)
    total = sq_out[...]
    for j in range(1, n):
        sums[j - 1].wait_recv()
        total = total + sq_in[j]
    column = jnp.transpose(jnp.broadcast_to(total[0:1, :], (128, tok_rows)))[:, 0:1]
    out[...] = (mixed * lax.rsqrt(column / depth + EPS) * final_gain[...]).astype(BF16)
    for copy in sent:
        copy.wait_send()


def shards(
    tokens, norm_gain, routing, route_weight, gate_weight, up_weight, down_weight, final_gain
):
    ep_count, n = lax.axis_size("ep"), lax.axis_size("tp")
    planes = ep_count // 2
    tok_rows, width = tokens.shape
    capacity = 2 * ((tok_rows * TOPK * 5 + planes * 8 - 1) // (planes * 8))
    cap = -(-capacity // 16) * 16
    groups = min(4, planes)
    per = planes // groups
    rows = per * cap
    depth, inner = gate_weight.shape[1:]
    dma = pltpu.SemaphoreType.DMA
    vmem, anywhere = pl.BlockSpec(memory_space=pltpu.VMEM), pl.BlockSpec(memory_space=pl.ANY)
    return pl.pallas_call(
        functools.partial(kernel, n, planes, groups),
        out_shape=jax.ShapeDtypeStruct((tok_rows, width), BF16),
        in_specs=[vmem] * 5 + [anywhere] * 3 + [vmem],
        out_specs=vmem,
        scratch_shapes=[
            pltpu.VMEM((depth, inner), BF16),
            pltpu.VMEM((depth, inner), BF16),
            pltpu.VMEM((n * inner, width), BF16),
            pltpu.VMEM((n, 1, width), F32),
            pltpu.VMEM((planes, cap, width), BF16),
            pltpu.VMEM((groups, n, 2, per, cap, width), BF16),
            pltpu.VMEM((2 * rows, depth), BF16),
            pltpu.VMEM((groups, n, 2, rows, inner), BF16),
            pltpu.VMEM((groups, rows, width), BF16),
            pltpu.VMEM((groups, rows, width), BF16),
            pltpu.VMEM((groups, rows, width), BF16),
            pltpu.VMEM((groups, per, cap, width), BF16),
            pltpu.VMEM((planes, cap, width), BF16),
            pltpu.VMEM((8, 128), F32),
            pltpu.VMEM((n, 8, 128), F32),
            dma((3,)), dma((n,)), dma((n,)), dma((planes,)), dma((planes,)),
            dma((groups, n)), dma((groups, n)), dma((groups, n)), dma((groups, n)),
            dma((groups, 2, n)), dma((groups, 2, n)), dma((groups,)), dma((groups,)),
            dma((planes,)), dma((planes,)), dma((n,)), dma((n,)),
        ],
        compiler_params=pltpu.CompilerParams(
            collective_id=0, has_side_effects=True, vmem_limit_bytes=60 * 1024 * 1024
        ),
    )(
        tokens, norm_gain.reshape(1, width), routing, routing.T, route_weight,
        gate_weight, up_weight, down_weight, final_gain.reshape(1, width),
    )


def solution(mesh):
    placed = (
        P("ep", "tp"),
        P("tp"),
        P("ep", None),
        P("ep", None),
        P("ep", None, "tp"),
        P("ep", None, "tp"),
        P("ep", None, "tp"),
        P("tp"),
    )
    return jax.shard_map(
        shards, mesh=mesh, in_specs=placed, out_specs=P("ep", "tp"), check_vma=False
    )
```

```python
import functools

import jax
import jax.numpy as jnp
from jax import lax
from jax.experimental import pallas as pl
from jax.experimental.pallas import tpu as pltpu
from jax.sharding import PartitionSpec as P

TOPK = 2
EPS = 1e-05
MESH = pl.DeviceIdType.MESH
F32, BF16 = jnp.float32, jnp.bfloat16


def flipped(index, mask):
    out, bit = index, 1
    while bit <= mask:
        if mask & bit:
            out = out + bit - 2 * bit * ((index // bit) % 2)
        bit *= 2
    return out


def dot(a, b):
    return jnp.dot(a, b, preferred_element_type=F32)


def dot_t(a, b):
    return lax.dot_general(a, b, (((0,), (0,)), ((), ())), preferred_element_type=F32)


def kernel(
    n, planes, groups,
    tokens, gain, routing_t, weight_t, gate_hbm, up_hbm, down_hbm, final_gain,
    out,
    wg, wu, wd, gains, picked, x, xn, hid, half_own, half_send, half_recv, pair, comb, sq_out, sq_in,
    w_sem, gain_s, gain_r, disp_s, disp_r, x_s, x_r, d2d_s, d2d_r, h_s, h_r, po_s, po_r, c_s, c_r,
    sq_s, sq_r,
):
    ep, t = lax.axis_index("ep"), lax.axis_index("tp")
    z, core = ep // 2, ep % 2
    partner = (ep + 1 - 2 * core, t)
    cap, width = picked.shape[1], picked.shape[2]
    per = planes // groups
    rows = per * cap
    inner = hid.shape[-1]
    tok_rows = tokens.shape[0]
    depth = n * width
    bits = [1 << b for b in range(n.bit_length() - 1)]
    tp_peer = [(ep, flipped(t, j)) for j in range(n)]
    tp_index = [flipped(t, j) for j in range(n)]
    expert = [flipped(z, k) for k in range(planes)]
    plane_peer = [(2 * expert[k] + core, t) for k in range(planes)]

    loads = [
        pltpu.make_async_copy(src.at[0], dst, w_sem.at[i])
        for i, (src, dst) in enumerate(((gate_hbm, wg), (up_hbm, wu), (down_hbm, wd)))
    ]
    for load in loads:
        load.start()

    barrier = pltpu.get_barrier_semaphore()
    peers = tp_peer[1:] + plane_peer[1:] + [partner]
    for peer in peers:
        pl.semaphore_signal(barrier, inc=1, device_id=peer, device_id_type=MESH)

    token_row = lax.broadcasted_iota(jnp.int32, (tok_rows, tok_rows), 0)
    token_col = lax.broadcasted_iota(jnp.int32, (tok_rows, tok_rows), 1)
    r_t0, r_t1 = routing_t[0:1, :], routing_t[1:2, :]
    wide = -(-planes // 16) * 16
    sub = lax.broadcasted_iota(jnp.int32, (wide, tok_rows), 0)
    member_t = jnp.zeros((wide, tok_rows), F32)
    for k in range(planes):
        named = ((r_t0 == expert[k]) | (r_t1 == expert[k])).astype(F32)
        member_t = jnp.where(sub == k, named, member_t)
    earlier = (token_row < token_col).astype(F32).astype(BF16)
    slot_t = dot(member_t.astype(BF16), earlier)
    slot_t = jnp.where(member_t > 0, slot_t, -1.0)
    slot_sub = lax.broadcasted_iota(jnp.int32, (cap, tok_rows), 0).astype(F32)

    def pick(k):
        chosen = (slot_sub == slot_t[k : k + 1, :]).astype(F32).astype(BF16)
        return dot(chosen, tokens[...]).astype(BF16)

    sent = []

    def remote(src, dst, s, r, peer):
        return pltpu.make_async_remote_copy(
            src_ref=src, dst_ref=dst, send_sem=s, recv_sem=r, device_id=peer, device_id_type=MESH
        )

    def start(copy):
        copy.start()
        sent.append(copy)
        return copy

    for k in range(1, planes):
        picked[k] = pick(k)
    x[0, 0, 0, 0] = pick(0)

    pl.semaphore_wait(barrier, len(peers))

    disp = [
        None if k == 0 else remote(
            picked.at[k], x.at[k // per, 0, 0, k % per], disp_s.at[k], disp_r.at[k], plane_peer[k]
        )
        for k in range(planes)
    ]
    for k in range(1, planes):
        start(disp[k])

    def tree(at, send_sem, recv_sem, order):
        copies, need = {}, {0: []}
        have = [0]
        for position, bit in enumerate(order):
            for j in list(have):
                into = j ^ bit
                copies[into] = remote(at(j), at(into), send_sem(into), recv_sem(into), tp_peer[bit])
                need[j].append(into)
                need[into] = []
                have.append(into)
        return copies, need, have[1:]

    def ascending(g):
        return bits if g % 2 == 0 else bits[::-1]

    trees = [
        tree(
            lambda j, g=g: x.at[g, j, 0], lambda j, g=g: x_s.at[g, j],
            lambda j, g=g: x_r.at[g, j], ascending(g),
        )
        for g in range(groups)
    ]
    across = [
        [remote(x.at[g, j, 0], x.at[g, j, 1], d2d_s.at[g, j], d2d_r.at[g, j], partner) for j in range(n)]
        for g in range(groups)
    ]
    hidden_trees = [
        [
            tree(
                lambda j, g=g, side=side: hid.at[g, j, side],
                lambda j, g=g, side=side: h_s.at[g, side, j],
                lambda j, g=g, side=side: h_r.at[g, side, j], ascending(side),
            )
            for side in range(2)
        ]
        for g in range(groups)
    ]

    def gather_start(g):
        for k in range(max(1, g * per), (g + 1) * per):
            disp[k].wait_recv()
        copies, need, _ = trees[g]
        for into in need[0]:
            start(copies[into])
        start(across[g][0])

    def gather_relay(g):
        copies, need, arrivals = trees[g]
        for j in arrivals:
            if need[j]:
                copies[j].wait_recv()
                for into in need[j]:
                    start(copies[into])
                start(across[g][j])

    def gather_end(g):
        copies, need, arrivals = trees[g]
        for j in arrivals:
            if not need[j]:
                copies[j].wait_recv()
                start(across[g][j])
        for j in range(n):
            across[g][j].wait_recv()

    def upward(g):
        parts = [x[g, j].reshape(2 * rows, width).astype(F32) for j in range(n)]
        square = sum(jnp.sum(p * p, axis=1, keepdims=True) for p in parts)
        scale = lax.rsqrt(square / depth + EPS)
        for j in range(n):
            columns = pl.ds(pl.multiple_of(tp_index[j] * width, width), width)
            xn[:, columns] = (parts[j] * scale * gains[j]).astype(BF16)
        for first in range(0, inner, 256):
            last = min(first + 256, inner)
            left = dot(xn[...], wg[:, first:last])
            right = dot(xn[...], wu[:, first:last])
            value = (jax.nn.silu(left) * right).astype(BF16)
            hid[g, 0, :, :, first:last] = value.reshape(2, rows, last - first)

    def hidden_start(g):
        for step in range(len(bits)):
            for side in range(2):
                copies, need, _ = hidden_trees[g][side]
                start(copies[need[0][step]])

    def hidden_relay(g):
        for side in range(2):
            copies, need, arrivals = hidden_trees[g][side]
            for j in arrivals:
                if need[j]:
                    copies[j].wait_recv()
                    for into in need[j]:
                        start(copies[into])

    halves = [
        remote(half_send.at[g], half_recv.at[g], po_s.at[g], po_r.at[g], partner) for g in range(groups)
    ]

    def downward(g):
        total = None
        for j in range(n):
            for side in range(2):
                copies, need, _ = hidden_trees[g][side]
                if j and not need[j]:
                    copies[j].wait_recv()
            part = wd[pl.ds(pl.multiple_of(tp_index[j] * inner, inner), inner), :]
            term = dot(hid[g, j].reshape(2 * rows, inner), part)
            total = term if total is None else total + term
        half_own[g] = total[:rows].astype(BF16)
        half_send[g] = total[rows:].astype(BF16)
        start(halves[g])

    back = [
        None if k == 0 else remote(
            pair.at[k // per, k % per], comb.at[k], c_s.at[k], c_r.at[k], plane_peer[k]
        )
        for k in range(planes)
    ]

    def combine(g):
        halves[g].wait_recv()
        both = (half_own[g].astype(F32) + half_recv[g].astype(F32)).astype(BF16)
        pair[g] = both.reshape(per, cap, width)
        for k in range(g * per, (g + 1) * per):
            if k == 0:
                comb[0] = both[:cap]
            else:
                start(back[k])

    gain_copies = [
        remote(gain, gains.at[j], gain_s.at[j], gain_r.at[j], tp_peer[j]) for j in range(1, n)
    ]
    gather_start(0)
    for copy in gain_copies:
        start(copy)
    gains[0] = gain[...]
    for g in range(1, groups):
        gather_start(g)
        gather_relay(g - 1)
    for copy in gain_copies:
        copy.wait_recv()
    loads[0].wait()
    loads[1].wait()
    for g in range(groups):
        gather_end(g)
        upward(g)
        if g == 0:
            gather_relay(groups - 1)
        hidden_start(g)
    loads[2].wait()
    turn = list(range(1, groups)) + [0]
    for g in turn:
        hidden_relay(g)
    for position, g in enumerate(turn):
        downward(g)
        if position:
            combine(turn[position - 1])

    w_t0, w_t1 = weight_t[0:1, :], weight_t[1:2, :]

    def share(k):
        weight = jnp.where(r_t0 == expert[k], w_t0, w_t1)
        table = jnp.where(slot_sub == slot_t[k : k + 1, :], weight, 0.0)
        high = table.astype(BF16)
        rest = table - high.astype(F32)
        middle = rest.astype(BF16)
        low = (rest - middle.astype(F32)).astype(BF16)
        block = comb[k]
        return dot_t(high, block) + (dot_t(middle, block) + dot_t(low, block))

    combine(turn[-1])
    mixed = None
    for k in list(range(1, planes)) + [0]:
        if k:
            back[k].wait_recv()
        mixed = share(k) if mixed is None else mixed + share(k)

    square = jnp.sum(mixed * mixed, axis=1, keepdims=True)
    sq_out[...] = jnp.transpose(jnp.broadcast_to(square, (tok_rows, 128)))[0:8, :]
    sums = [remote(sq_out, sq_in.at[j], sq_s.at[j], sq_r.at[j], tp_peer[j]) for j in range(1, n)]
    for copy in sums:
        start(copy)
    total = sq_out[...]
    for j in range(1, n):
        sums[j - 1].wait_recv()
        total = total + sq_in[j]
    column = jnp.transpose(jnp.broadcast_to(total[0:1, :], (128, tok_rows)))[:, 0:1]
    out[...] = (mixed * lax.rsqrt(column / depth + EPS) * final_gain[...]).astype(BF16)
    for copy in sent:
        copy.wait_send()


def shards(
    tokens, norm_gain, routing, route_weight, gate_weight, up_weight, down_weight, final_gain
):
    ep_count, n = lax.axis_size("ep"), lax.axis_size("tp")
    planes = ep_count // 2
    tok_rows, width = tokens.shape
    capacity = 2 * ((tok_rows * TOPK * 5 + planes * 8 - 1) // (planes * 8))
    cap = -(-capacity // 16) * 16
    groups = min(4, planes)
    per = planes // groups
    rows = per * cap
    depth, inner = gate_weight.shape[1:]
    dma = pltpu.SemaphoreType.DMA
    vmem, anywhere = pl.BlockSpec(memory_space=pltpu.VMEM), pl.BlockSpec(memory_space=pl.ANY)
    return pl.pallas_call(
        functools.partial(kernel, n, planes, groups),
        out_shape=jax.ShapeDtypeStruct((tok_rows, width), BF16),
        in_specs=[vmem] * 4 + [anywhere] * 3 + [vmem],
        out_specs=vmem,
        scratch_shapes=[
            pltpu.VMEM((depth, inner), BF16),
            pltpu.VMEM((depth, inner), BF16),
            pltpu.VMEM((n * inner, width), BF16),
            pltpu.VMEM((n, 1, width), F32),
            pltpu.VMEM((planes, cap, width), BF16),
            pltpu.VMEM((groups, n, 2, per, cap, width), BF16),
            pltpu.VMEM((2 * rows, depth), BF16),
            pltpu.VMEM((groups, n, 2, rows, inner), BF16),
            pltpu.VMEM((groups, rows, width), BF16),
            pltpu.VMEM((groups, rows, width), BF16),
            pltpu.VMEM((groups, rows, width), BF16),
            pltpu.VMEM((groups, per, cap, width), BF16),
            pltpu.VMEM((planes, cap, width), BF16),
            pltpu.VMEM((8, 128), F32),
            pltpu.VMEM((n, 8, 128), F32),
            dma((3,)), dma((n,)), dma((n,)), dma((planes,)), dma((planes,)),
            dma((groups, n)), dma((groups, n)), dma((groups, n)), dma((groups, n)),
            dma((groups, 2, n)), dma((groups, 2, n)), dma((groups,)), dma((groups,)),
            dma((planes,)), dma((planes,)), dma((n,)), dma((n,)),
        ],
        compiler_params=pltpu.CompilerParams(
            collective_id=0, has_side_effects=True, vmem_limit_bytes=60 * 1024 * 1024
        ),
    )(
        tokens, norm_gain.reshape(1, width), routing.T, route_weight.T,
        gate_weight, up_weight, down_weight, final_gain.reshape(1, width),
    )


def solution(mesh):
    placed = (
        P("ep", "tp"),
        P("tp"),
        P("ep", None),
        P("ep", None),
        P("ep", None, "tp"),
        P("ep", None, "tp"),
        P("ep", None, "tp"),
        P("tp"),
    )
    return jax.shard_map(
        shards, mesh=mesh, in_specs=placed, out_specs=P("ep", "tp"), check_vma=False
    )
```

```python
import functools

import jax
import jax.numpy as jnp
from jax import lax
from jax.experimental import pallas as pl
from jax.experimental.pallas import tpu as pltpu
from jax.sharding import PartitionSpec as P

TOPK = 2
EPS = 1e-05
MESH = pl.DeviceIdType.MESH
F32, BF16 = jnp.float32, jnp.bfloat16


def flipped(index, mask):
    out, bit = index, 1
    while bit <= mask:
        if mask & bit:
            out = out + bit - 2 * bit * ((index // bit) % 2)
        bit *= 2
    return out


def dot(a, b):
    return jnp.dot(a, b, preferred_element_type=F32)


def dot_t(a, b):
    return lax.dot_general(a, b, (((0,), (0,)), ((), ())), preferred_element_type=F32)


def kernel(
    n, planes, groups,
    tokens, gain, routing_t, weight_t, gate_hbm, up_hbm, down_hbm,
    out,
    wg, wu, wd, gains, picked, x, xn, hid, half_own, half_send, half_recv, pair, comb, sq_out, sq_in,
    w_sem, gain_s, gain_r, disp_s, disp_r, x_s, x_r, d2d_s, d2d_r, h_s, h_r, po_s, po_r, c_s, c_r,
    sq_s, sq_r,
):
    ep, t = lax.axis_index("ep"), lax.axis_index("tp")
    z, core = ep // 2, ep % 2
    partner = (ep + 1 - 2 * core, t)
    cap, width = picked.shape[1], picked.shape[2]
    per = planes // groups
    rows = per * cap
    inner = hid.shape[-1]
    tok_rows = tokens.shape[0]
    depth = n * width
    bits = [1 << b for b in range(n.bit_length() - 1)]
    tp_peer = [(ep, flipped(t, j)) for j in range(n)]
    tp_index = [flipped(t, j) for j in range(n)]
    expert = [flipped(z, k) for k in range(planes)]
    plane_peer = [(2 * expert[k] + core, t) for k in range(planes)]

    loads = [
        pltpu.make_async_copy(src.at[0], dst, w_sem.at[i])
        for i, (src, dst) in enumerate(((gate_hbm, wg), (up_hbm, wu), (down_hbm, wd)))
    ]
    for load in loads:
        load.start()

    barrier = pltpu.get_barrier_semaphore()
    peers = tp_peer[1:] + plane_peer[1:] + [partner]
    for peer in peers:
        pl.semaphore_signal(barrier, inc=1, device_id=peer, device_id_type=MESH)

    token_row = lax.broadcasted_iota(jnp.int32, (tok_rows, tok_rows), 0)
    token_col = lax.broadcasted_iota(jnp.int32, (tok_rows, tok_rows), 1)
    r_t0, r_t1 = routing_t[0:1, :], routing_t[1:2, :]
    wide = -(-planes // 16) * 16
    sub = lax.broadcasted_iota(jnp.int32, (wide, tok_rows), 0)
    member_t = jnp.zeros((wide, tok_rows), F32)
    for k in range(planes):
        named = ((r_t0 == expert[k]) | (r_t1 == expert[k])).astype(F32)
        member_t = jnp.where(sub == k, named, member_t)
    earlier = (token_row < token_col).astype(F32).astype(BF16)
    slot_t = dot(member_t.astype(BF16), earlier)
    slot_t = jnp.where(member_t > 0, slot_t, -1.0)
    slot_sub = lax.broadcasted_iota(jnp.int32, (cap, tok_rows), 0).astype(F32)

    def pick(k):
        chosen = (slot_sub == slot_t[k : k + 1, :]).astype(F32).astype(BF16)
        return dot(chosen, tokens[...]).astype(BF16)

    sent = []

    def remote(src, dst, s, r, peer):
        return pltpu.make_async_remote_copy(
            src_ref=src, dst_ref=dst, send_sem=s, recv_sem=r, device_id=peer, device_id_type=MESH
        )

    def start(copy):
        copy.start()
        sent.append(copy)
        return copy

    for k in range(1, planes):
        picked[k] = pick(k)
    x[0, 0, 0, 0] = pick(0)

    pl.semaphore_wait(barrier, len(peers))

    disp = [
        None if k == 0 else remote(
            picked.at[k], x.at[k // per, 0, 0, k % per], disp_s.at[k], disp_r.at[k], plane_peer[k]
        )
        for k in range(planes)
    ]
    for k in range(1, planes):
        start(disp[k])

    def tree(at, send_sem, recv_sem, order):
        copies, need = {}, {0: []}
        have = [0]
        for position, bit in enumerate(order):
            for j in list(have):
                into = j ^ bit
                copies[into] = remote(at(j), at(into), send_sem(into), recv_sem(into), tp_peer[bit])
                need[j].append(into)
                need[into] = []
                have.append(into)
        return copies, need, have[1:]

    def ascending(g):
        return bits if g % 2 == 0 else bits[::-1]

    trees = [
        tree(
            lambda j, g=g: x.at[g, j, 0], lambda j, g=g: x_s.at[g, j],
            lambda j, g=g: x_r.at[g, j], ascending(g),
        )
        for g in range(groups)
    ]
    across = [
        [remote(x.at[g, j, 0], x.at[g, j, 1], d2d_s.at[g, j], d2d_r.at[g, j], partner) for j in range(n)]
        for g in range(groups)
    ]
    hidden_trees = [
        [
            tree(
                lambda j, g=g, side=side: hid.at[g, j, side],
                lambda j, g=g, side=side: h_s.at[g, side, j],
                lambda j, g=g, side=side: h_r.at[g, side, j], ascending(side),
            )
            for side in range(2)
        ]
        for g in range(groups)
    ]

    def gather_start(g):
        for k in range(max(1, g * per), (g + 1) * per):
            disp[k].wait_recv()
        copies, need, _ = trees[g]
        for into in need[0]:
            start(copies[into])
        start(across[g][0])

    def gather_relay(g):
        copies, need, arrivals = trees[g]
        for j in arrivals:
            if need[j]:
                copies[j].wait_recv()
                for into in need[j]:
                    start(copies[into])
                start(across[g][j])

    def gather_end(g):
        copies, need, arrivals = trees[g]
        for j in arrivals:
            if not need[j]:
                copies[j].wait_recv()
                start(across[g][j])
        for j in range(n):
            across[g][j].wait_recv()

    def upward(g):
        parts = [x[g, j].reshape(2 * rows, width).astype(F32) for j in range(n)]
        square = sum(jnp.sum(p * p, axis=1, keepdims=True) for p in parts)
        scale = lax.rsqrt(square / depth + EPS)
        for j in range(n):
            columns = pl.ds(pl.multiple_of(tp_index[j] * width, width), width)
            xn[:, columns] = (parts[j] * scale * gains[j]).astype(BF16)
        for first in range(0, inner, 256):
            last = min(first + 256, inner)
            left = dot(xn[...], wg[:, first:last])
            right = dot(xn[...], wu[:, first:last])
            value = (jax.nn.silu(left) * right).astype(BF16)
            hid[g, 0, :, :, first:last] = value.reshape(2, rows, last - first)

    def hidden_start(g):
        for step in range(len(bits)):
            for side in range(2):
                copies, need, _ = hidden_trees[g][side]
                start(copies[need[0][step]])

    def hidden_relay(g):
        for side in range(2):
            copies, need, arrivals = hidden_trees[g][side]
            for j in arrivals:
                if need[j]:
                    copies[j].wait_recv()
                    for into in need[j]:
                        start(copies[into])

    halves = [
        remote(half_send.at[g], half_recv.at[g], po_s.at[g], po_r.at[g], partner) for g in range(groups)
    ]

    def downward(g):
        total = None
        for j in range(n):
            for side in range(2):
                copies, need, _ = hidden_trees[g][side]
                if j and not need[j]:
                    copies[j].wait_recv()
            part = wd[pl.ds(pl.multiple_of(tp_index[j] * inner, inner), inner), :]
            term = dot(hid[g, j].reshape(2 * rows, inner), part)
            total = term if total is None else total + term
        half_own[g] = total[:rows].astype(BF16)
        half_send[g] = total[rows:].astype(BF16)
        start(halves[g])

    back = [
        None if k == 0 else remote(
            pair.at[k // per, k % per], comb.at[k], c_s.at[k], c_r.at[k], plane_peer[k]
        )
        for k in range(planes)
    ]

    def combine(g):
        halves[g].wait_recv()
        both = (half_own[g].astype(F32) + half_recv[g].astype(F32)).astype(BF16)
        pair[g] = both.reshape(per, cap, width)
        for k in range(g * per, (g + 1) * per):
            if k == 0:
                comb[0] = both[:cap]
            else:
                start(back[k])

    gain_copies = [
        remote(gain, gains.at[j], gain_s.at[j], gain_r.at[j], tp_peer[j]) for j in range(1, n)
    ]
    gather_start(0)
    for copy in gain_copies:
        start(copy)
    gains[0] = gain[...]
    gather_relay(0)
    for g in range(1, min(3, groups)):
        gather_start(g)
    for copy in gain_copies:
        copy.wait_recv()
    loads[0].wait()
    loads[1].wait()
    for g in range(groups):
        gather_end(g)
        upward(g)
        if g == 0:
            for later in range(1, groups):
                if later >= 3:
                    gather_start(later)
                if later == 1:
                    gather_relay(1)
        hidden_start(g)
        if g + 2 < groups:
            gather_relay(g + 2)
    loads[2].wait()
    turn = list(range(1, groups)) + [0]
    for g in turn:
        hidden_relay(g)
    for position, g in enumerate(turn):
        downward(g)
        if position:
            combine(turn[position - 1])

    w_t0, w_t1 = weight_t[0:1, :], weight_t[1:2, :]

    def share(k):
        weight = jnp.where(r_t0 == expert[k], w_t0, w_t1)
        table = jnp.where(slot_sub == slot_t[k : k + 1, :], weight, 0.0)
        high = table.astype(BF16)
        rest = table - high.astype(F32)
        middle = rest.astype(BF16)
        low = (rest - middle.astype(F32)).astype(BF16)
        block = comb[k]
        return dot_t(high, block) + (dot_t(middle, block) + dot_t(low, block))

    combine(turn[-1])
    mixed = None
    for k in list(range(1, planes)) + [0]:
        if k:
            back[k].wait_recv()
        mixed = share(k) if mixed is None else mixed + share(k)

    square = jnp.sum(mixed * mixed, axis=1, keepdims=True)
    sq_out[...] = jnp.transpose(jnp.broadcast_to(square, (tok_rows, 128)))[0:8, :]
    sums = [remote(sq_out, sq_in.at[j], sq_s.at[j], sq_r.at[j], tp_peer[j]) for j in range(1, n)]
    for copy in sums:
        start(copy)
    total = sq_out[...]
    for j in range(1, n):
        sums[j - 1].wait_recv()
        total = total + sq_in[j]
    column = jnp.transpose(jnp.broadcast_to(total[0:1, :], (128, tok_rows)))[:, 0:1]
    out[...] = mixed * lax.rsqrt(column / depth + EPS)
    for copy in sent:
        copy.wait_send()


def shards(
    tokens, norm_gain, routing, route_weight, gate_weight, up_weight, down_weight, final_gain
):
    ep_count, n = lax.axis_size("ep"), lax.axis_size("tp")
    planes = ep_count // 2
    tok_rows, width = tokens.shape
    capacity = 2 * ((tok_rows * TOPK * 5 + planes * 8 - 1) // (planes * 8))
    cap = -(-capacity // 16) * 16
    groups = min(4, planes)
    per = planes // groups
    rows = per * cap
    depth, inner = gate_weight.shape[1:]
    dma = pltpu.SemaphoreType.DMA
    vmem, anywhere = pl.BlockSpec(memory_space=pltpu.VMEM), pl.BlockSpec(memory_space=pl.ANY)
    scaled = pl.pallas_call(
        functools.partial(kernel, n, planes, groups),
        out_shape=jax.ShapeDtypeStruct((tok_rows, width), F32),
        in_specs=[vmem] * 4 + [anywhere] * 3,
        out_specs=vmem,
        scratch_shapes=[
            pltpu.VMEM((depth, inner), BF16),
            pltpu.VMEM((depth, inner), BF16),
            pltpu.VMEM((n * inner, width), BF16),
            pltpu.VMEM((n, 1, width), F32),
            pltpu.VMEM((planes, cap, width), BF16),
            pltpu.VMEM((groups, n, 2, per, cap, width), BF16),
            pltpu.VMEM((2 * rows, depth), BF16),
            pltpu.VMEM((groups, n, 2, rows, inner), BF16),
            pltpu.VMEM((groups, rows, width), BF16),
            pltpu.VMEM((groups, rows, width), BF16),
            pltpu.VMEM((groups, rows, width), BF16),
            pltpu.VMEM((groups, per, cap, width), BF16),
            pltpu.VMEM((planes, cap, width), BF16),
            pltpu.VMEM((8, 128), F32),
            pltpu.VMEM((n, 8, 128), F32),
            dma((3,)), dma((n,)), dma((n,)), dma((planes,)), dma((planes,)),
            dma((groups, n)), dma((groups, n)), dma((groups, n)), dma((groups, n)),
            dma((groups, 2, n)), dma((groups, 2, n)), dma((groups,)), dma((groups,)),
            dma((planes,)), dma((planes,)), dma((n,)), dma((n,)),
        ],
        compiler_params=pltpu.CompilerParams(
            collective_id=0, has_side_effects=True, vmem_limit_bytes=60 * 1024 * 1024
        ),
    )(
        tokens, norm_gain.reshape(1, width), routing.T, route_weight.T,
        gate_weight, up_weight, down_weight,
    )
    return (scaled * final_gain).astype(BF16)


def solution(mesh):
    placed = (
        P("ep", "tp"),
        P("tp"),
        P("ep", None),
        P("ep", None),
        P("ep", None, "tp"),
        P("ep", None, "tp"),
        P("ep", None, "tp"),
        P("tp"),
    )
    return jax.shard_map(
        shards, mesh=mesh, in_specs=placed, out_specs=P("ep", "tp"), check_vma=False
    )
```
